32 devices in a mesh: sp: 8 (over z, y), tp: 4 (over x, core).
Axes of the slice: x: 2, y: 2, z: 4, core: 2. Of those that a mesh axis runs over, the one named last changes fastest.
Arguments:
- tokens: bfloat16 [2048, 4096], P(('sp', 'tp')), may hold values from -6 to 6
- norm_gain: float32 [4096], replicated, may hold values from 0.1 to 1.9
- w_query: bfloat16 [4096, 1024], P(None, 'tp'), may hold values from -0.25 to 0.25
- w_key: bfloat16 [4096, 512], P(None, 'tp'), may hold values from -0.09375 to 0.09375
- w_value: bfloat16 [4096, 512], P(None, 'tp'), may hold values from -0.09375 to 0.09375
- score_shift: float32 [8], P('tp'), may hold values from -15 to -8
- w_conv_b: bfloat16 [4096, 1024], P(None, 'tp'), may hold values from -0.09375 to 0.09375
- w_conv_c: bfloat16 [4096, 1024], P(None, 'tp'), may hold values from -0.09375 to 0.09375
- w_conv_u: bfloat16 [4096, 1024], P(None, 'tp'), may hold values from -0.09375 to 0.09375
- conv_kernel: float32 [3, 1024], P(None, 'tp'), may hold values from -3.5 to 3.5
- w_out_att: bfloat16 [4096, 1024], P('sp', 'tp'), may hold values from -0.75 to 0.75
- w_out_conv: bfloat16 [4096, 1024], P('sp', 'tp'), may hold values from -0.1875 to 0.1875
Outputs:
- mixed: bfloat16 [2048, 4096], P(('sp', 'tp'))
- log_weight: float32 [2048, 8], P('sp', 'tp')
The draws below stay inside these ranges and needn't reach their ends.
All inputs are finite; a program needn't handle non-finite values.
Results may differ from the reference program's by a relative error of at most 0.017.
Values may be sent and summed in bfloat16 or wider, within the bound.
A program may use at most 128 MiB of HBM per device.

```python
import jax
import jax.numpy as jnp
from jax import lax

D = 4096
ATT_HEADS = 8
KV_HEADS = 4
HEAD_DIM = 128
CONV_W = 1024
CONV_K = 3
KEY_BLOCK = 1024
TOK_DEV = 256
ATT_W = 1024
TOKENS = 2048
N_TP = 4


def draw_score_shift(key, part):
    return jax.random.uniform(key, (ATT_HEADS,), jnp.float32, -13.0, -8.0)


def levels(rng, extent, shards, low, high):
    factor_of, own = 1.0, jax.random.fold_in(rng, 6)
    for position, blocks in shards:
        heights = jnp.exp(jax.random.uniform(jax.random.fold_in(own, position), (blocks,), jnp.float32, low / len(shards), high / len(shards)))
        factor_of = factor_of * jnp.repeat(heights, extent[position] // blocks).reshape([-1 if axis == position else 1 for axis in range(len(extent))])
    return factor_of


def bell_draw(key, extent, spread, most, split=(), kind=jnp.bfloat16):
    gain = levels(key, extent, split, -0.22, 0.18) if split else 1.0
    entries = jax.random.normal(key, extent, jnp.float32) * spread * gain
    return jnp.minimum(jnp.maximum(entries, -most), most).astype(kind)


def setup_inputs(seed: int = 0) -> dict:
    splits = jax.random.split(jax.random.key(seed), 13)
    tokens = bell_draw(splits[0], (TOKENS, D), 1.0, 6.0, ((0, 32),))
    norm_gain = jnp.clip(1.0 + 0.18 * jax.random.normal(splits[1], (D,), jnp.float32), 0.1, 1.9)
    w_query = bell_draw(splits[2], (D, ATT_W), (D // 9) ** -0.5, 0.25, ((1, 4),))
    w_key = bell_draw(splits[3], (D, KV_HEADS * HEAD_DIM), D ** -0.5, 0.09375, ((1, 4),))
    w_value = bell_draw(splits[4], (D, KV_HEADS * HEAD_DIM), D ** -0.5, 0.09375, ((1, 4),))
    score_shift = draw_score_shift(jax.random.fold_in(splits[12], 71), 0)
    w_conv_b = bell_draw(splits[6], (D, CONV_W), D ** -0.5, 0.09375, ((1, 4),))
    w_conv_c = bell_draw(splits[7], (D, CONV_W), D ** -0.5, 0.09375, ((1, 4),))
    w_conv_u = bell_draw(splits[8], (D, CONV_W), D ** -0.5, 0.09375, ((1, 4),))
    conv_kernel = bell_draw(splits[9], (CONV_K, CONV_W), CONV_K ** -0.5, 3.5, ((1, 4),), jnp.float32)
    w_out_att = bell_draw(splits[10], (D, ATT_W), (ATT_W // 16) ** -0.5, 0.75, ((0, 8), (1, 4)))
    w_out_conv = bell_draw(splits[11], (D, CONV_W), CONV_W ** -0.5, 0.1875, ((0, 8), (1, 4)))
    return {"tokens": tokens, "norm_gain": norm_gain, "w_query": w_query, "w_key": w_key, "w_value": w_value, "score_shift": score_shift, "w_conv_b": w_conv_b, "w_conv_c": w_conv_c, "w_conv_u": w_conv_u, "conv_kernel": conv_kernel, "w_out_att": w_out_att, "w_out_conv": w_out_conv}


def normalize(tokens, norm_gain):
    widened = tokens.astype(jnp.float32)
    inverse = lax.rsqrt(lax.optimization_barrier(jnp.mean(widened * widened, axis=-1, keepdims=True)) + 1e-06)
    return (widened * inverse * norm_gain).astype(jnp.bfloat16)

def block_terms(grouped_q, key_block, value_block, shifts, query_pos, key_first):
    scores = jnp.einsum('qhgd,khd->qhgk', grouped_q.astype(jnp.float32), key_block.astype(jnp.float32))
    scores = scores * HEAD_DIM ** (-0.5) + shifts[None, :, :, None]
    key_pos = key_first + jnp.arange(KEY_BLOCK, dtype=jnp.int32)
    causal = key_pos[None, None, None, :] < query_pos[:, None, None, None]
    soft = jnp.where(causal, jax.nn.softplus(scores), 0.0)
    after_sum = lax.cumsum(soft, axis=3, reverse=True) - soft
    relative = jnp.where(causal, jnp.exp(jax.nn.log_sigmoid(scores) - after_sum), 0.0).astype(jnp.bfloat16)
    partial_value = jnp.einsum('qhgk,khd->qhgd', relative.astype(jnp.float32), value_block.astype(jnp.float32))
    return (partial_value, lax.optimization_barrier(jnp.sum(soft, axis=3)))

def reference(tokens, norm_gain, w_query, w_key, w_value, score_shift, w_conv_b, w_conv_c, w_conv_u, conv_kernel, w_out_att, w_out_conv):
    normed = normalize(tokens, norm_gain)

    def project(weight):
        return jnp.dot(normed, weight, preferred_element_type=jnp.float32).astype(jnp.bfloat16)
    queries = project(w_query)
    keys = project(w_key)
    values = project(w_value)
    gate_b = project(w_conv_b)
    gate_c = project(w_conv_c)
    inputs_u = project(w_conv_u)
    grouping = ATT_HEADS // KV_HEADS
    shifts = score_shift.reshape(KV_HEADS, grouping)
    key_blocks = keys.reshape(TOKENS // KEY_BLOCK, KEY_BLOCK, KV_HEADS, HEAD_DIM)
    value_blocks = values.reshape(TOKENS // KEY_BLOCK, KEY_BLOCK, KV_HEADS, HEAD_DIM)
    key_firsts = jnp.arange(TOKENS // KEY_BLOCK, dtype=jnp.int32) * KEY_BLOCK
    query_blocks = queries.reshape(TOKENS // TOK_DEV, TOK_DEV, KV_HEADS, grouping, HEAD_DIM)
    query_firsts = jnp.arange(TOKENS // TOK_DEV, dtype=jnp.int32) * TOK_DEV

    def per_query(inputs):
        grouped_q, query_first = inputs
        query_pos = query_first + jnp.arange(TOK_DEV, dtype=jnp.int32)

        def per_key(key_inputs):
            key_block, value_block, key_first = key_inputs
            return block_terms(grouped_q, key_block, value_block, shifts, query_pos, key_first)
        partials, totals = lax.map(per_key, (key_blocks, value_blocks, key_firsts))
        later_sum = lax.cumsum(totals, axis=0, reverse=True) - totals
        attended = lax.optimization_barrier(jnp.sum(jnp.exp(-later_sum)[..., None] * partials, axis=0))
        sums_all = lax.optimization_barrier(jnp.sum(totals, axis=0))
        return (attended.reshape(TOK_DEV, ATT_W), sums_all.reshape(TOK_DEV, ATT_HEADS))
    attended, sums_all = lax.map(per_query, (query_blocks, query_firsts))
    attended = attended.reshape(TOKENS, ATT_W).astype(jnp.bfloat16)
    log_weight = jnp.log(jnp.maximum(-jnp.expm1(-sums_all.reshape(TOKENS, ATT_HEADS)), 0.05))
    products = (gate_c.astype(jnp.float32) * inputs_u.astype(jnp.float32)).astype(jnp.bfloat16)
    padded = jnp.concatenate([jnp.zeros((CONV_K - 1, CONV_W), jnp.bfloat16), products], axis=0)
    summed = jnp.zeros((TOKENS, CONV_W), jnp.float32)
    for tap in range(CONV_K):
        summed = summed + conv_kernel[tap][None, :] * padded[tap:tap + TOKENS].astype(jnp.float32)
    convolved = (gate_b.astype(jnp.float32) * summed).astype(jnp.bfloat16)
    att_cols = ATT_W // N_TP
    conv_cols = CONV_W // N_TP
    contract = (((1,), (1,)), ((), ()))
    mixed_sum = jnp.zeros((TOKENS, D), jnp.float32)
    for shard_no in range(N_TP):
        att_part = attended[:, shard_no * att_cols:(shard_no + 1) * att_cols]
        att_rows = w_out_att[:, shard_no * att_cols:(shard_no + 1) * att_cols]
        conv_part = convolved[:, shard_no * conv_cols:(shard_no + 1) * conv_cols]
        conv_rows = w_out_conv[:, shard_no * conv_cols:(shard_no + 1) * conv_cols]
        share = lax.dot_general(att_part, att_rows, contract, preferred_element_type=jnp.float32)
        share = share + lax.dot_general(conv_part, conv_rows, contract, preferred_element_type=jnp.float32)
        mixed_sum = mixed_sum + share.astype(jnp.bfloat16).astype(jnp.float32)
    return (mixed_sum.astype(jnp.bfloat16), log_weight)
```

```python
import functools

import jax
import jax.numpy as jnp
from jax import lax
from jax.experimental import pallas as pl
from jax.experimental.pallas import tpu as pltpu
from jax.sharding import PartitionSpec as P

HEAD_DIM = 128
CONV_K = 3
HALO = 16
F32 = jnp.float32
BF16 = jnp.bfloat16
MESH = pl.DeviceIdType.MESH
NT = (((1,), (1,)), ((), ()))


def softplus(z):
    u = jnp.exp(-jnp.abs(z))
    small = u * (1.0 - u * (0.5 - u * (1.0 / 3.0 - u * 0.25)))
    return jnp.maximum(z, 0.0) + jnp.where(u < 0.01, small, jnp.log(1.0 + u))


def kernel(
    n,
    tok_ref, gain_ref, wq_hbm, wk_hbm, wv_hbm, shift_ref, wb_hbm, wc_hbm, wu_hbm, taps_ref, woa_ref, woc_ref,
    out_ref, logw_ref,
    wq, wk, wv, wb, wc, wu, xall, normed, q_sc, kv, wo, gate_sc, prod_sc, prev, ext, attn, conv,
    snd, keep, d2d, xsnd, xrcv,
    load_sem, tok_ssem, tok_rsem, kv_sem, w_sem, halo_sem, d2d_sem, x_sem,
):
    sp = lax.axis_index("sp")
    t = lax.axis_index("tp")
    near = t + 1 - 2 * (t % 2)
    far = t + 2 - 4 * ((t // 2) % 2)
    diag = near + 2 - 4 * ((near // 2) % 2)
    pos = jnp.where(sp % 2 == 0, sp // 2, n - 1 - sp // 2)

    def ring(place):
        place = (place + 2 * n) % n
        return jnp.where(place < n // 2, 2 * place, 2 * (n - 1 - place) + 1)

    right, left = ring(pos + 1), ring(pos - 1)
    following, leading = (sp + 1) % n, (sp + n - 1) % n
    rows = tok_ref.shape[0]
    toks = 4 * rows
    half = rows // 2
    heads = q_sc.shape[1] // HEAD_DIM
    kv_cols = kv.shape[3]
    grouping = heads // (kv_cols // HEAD_DIM)

    loads = [
        pltpu.make_async_copy(src, dst, load_sem.at[i])
        for i, (src, dst) in enumerate(
            ((wk_hbm, wk), (wv_hbm, wv), (wq_hbm, wq), (wc_hbm, wc), (wu_hbm, wu), (wb_hbm, wb))
        )
    ]
    barrier = pltpu.get_barrier_semaphore()
    for place in (right, left, following, leading):
        pl.semaphore_signal(barrier, inc=1, device_id={"sp": place}, device_id_type=MESH)
    for place in (near, far):
        pl.semaphore_signal(barrier, inc=1, device_id={"tp": place}, device_id_type=MESH)
    for load in loads:
        load.start()
    pl.semaphore_wait(barrier, 6)

    def push(src, dst, ssem, rsem, who):
        return pltpu.make_async_remote_copy(
            src_ref=src, dst_ref=dst, send_sem=ssem, recv_sem=rsem, device_id=who, device_id_type=MESH
        )

    to_far = [
        push(tok_ref.at[pl.ds(c * half, half)], xall.at[t, pl.ds(c * half, half)], tok_ssem.at[c], tok_rsem.at[c], {"tp": far})
        for c in range(2)
    ]
    to_near = push(tok_ref, xall.at[t], tok_ssem.at[2], tok_rsem.at[2], {"tp": near})
    relay = [
        push(xall.at[far, pl.ds(c * half, half)], xall.at[far, pl.ds(c * half, half)], tok_ssem.at[3 + c], tok_rsem.at[3 + c], {"tp": near})
        for c in range(2)
    ]
    for copy in to_far:
        copy.start()
    to_near.start()

    def hop(buf, sem, way, k, own):
        step, chunk = k // 2 + 1, k % 2 if way == 0 else 1 - k % 2
        block = ring(pos - (step - 1)) if way == 0 else ring(pos + (step - 1))
        src = own[chunk] if (own is not None and step == 1) else buf.at[block, chunk]
        who = right if way == 0 else left
        return push(src, buf.at[block, chunk], sem.at[0, way, k], sem.at[1, way, k], {"sp": who})

    def open_ring(buf, sem, own):
        for k in range(min(2, n - 1)):
            for way in range(2):
                hop(buf, sem, way, k, own).start()

    def serve(buf, sem, own, step):
        for k in (2 * step - 2, 2 * step - 1):
            if k <= n - 2:
                for way in range(2):
                    hop(buf, sem, way, k, own).wait_recv()
                    if k + 2 <= n - 2:
                        hop(buf, sem, way, k + 2, own).start()

    own_w = (woa_ref, woc_ref)
    open_ring(wo, w_sem, own_w)

    def project(groups, offset):
        for i, g in enumerate(groups):
            x = (tok_ref[...] if g is None else xall[g]).astype(F32)
            inverse = lax.rsqrt(jnp.mean(x * x, axis=-1, keepdims=True) + 1e-06)
            normed[pl.ds(i * rows, rows)] = (x * inverse * gain_ref[...]).astype(BF16)
        a = normed[...]

        def dot(w):
            return jnp.dot(a, w[...], preferred_element_type=F32).astype(BF16)

        def put(dst, value):
            for i, g in enumerate(groups):
                g = t if g is None else g
                dst[pl.ds(pl.multiple_of(g * rows, rows), rows)] = value[i * rows : (i + 1) * rows]

        if offset:
            pass
        else:
            for load in loads:
                load.wait()
        put(kv.at[sp, 0], dot(wk))
        put(kv.at[sp, 1], dot(wv))
        put(q_sc, dot(wq))
        put(prod_sc, (dot(wc).astype(F32) * dot(wu).astype(F32)).astype(BF16))
        put(gate_sc, dot(wb))

    to_near.wait_recv()
    project((None, near), 0)
    for c in range(2):
        to_far[c].wait_recv()
        relay[c].start()
    serve(wo, w_sem, own_w, 1)
    for c in range(2):
        relay[c].wait_recv()
    project((far, diag), 1)
    open_ring(kv, kv_sem, None)
    halo = push(prod_sc.at[pl.ds(toks - HALO, HALO)], prev, halo_sem.at[0], halo_sem.at[1], {"sp": following})
    halo.start()

    halo.wait_recv()
    ext[pl.ds(HALO, toks)] = prod_sc[...].astype(F32)
    ext[pl.ds(0, HALO)] = jnp.where(sp == 0, 0.0, prev[...].astype(F32))
    summed = jnp.zeros((toks, ext.shape[1]), F32)
    for tap in range(CONV_K):
        summed = summed + taps_ref[tap : tap + 1, :] * ext[pl.ds(HALO - (CONV_K - 1) + tap, toks)]
    ext[pl.ds(HALO, toks)] = gate_sc[...].astype(F32) * summed
    order = (t, far, near, diag)
    for i, g in enumerate(order):
        conv[pl.ds(i * rows, rows)] = ext[pl.ds(pl.multiple_of(HALO + g * rows, HALO), rows)].astype(BF16)

    for step in range(1, n // 2 + 1):
        serve(kv, kv_sem, None, step)
    if n // 2 >= 2:
        serve(wo, w_sem, own_w, 2)

    key_i = lax.broadcasted_iota(jnp.int32, (toks, toks), 0)
    key_j = lax.broadcasted_iota(jnp.int32, (toks, toks), 1)
    later = (key_i > key_j).astype(F32).astype(BF16)
    causal = key_j < key_i
    scale = HEAD_DIM ** (-0.5)
    for h in range(heads):
        cols = pl.ds(h * HEAD_DIM, HEAD_DIM)
        kv_at = pl.ds((h // grouping) * HEAD_DIM, HEAD_DIM)
        q = q_sc[:, cols]
        shift = shift_ref[0, h]

        def visit(slot, masked, acc, suffix, q=q, shift=shift, kv_at=kv_at):
            z = lax.dot_general(q, kv[slot, 0, :, kv_at], NT, preferred_element_type=F32) * scale + shift
            soft = softplus(z)
            if masked:
                soft = jnp.where(causal, soft, 0.0)
            high = soft.astype(BF16)
            low = (soft - high.astype(F32)).astype(BF16)
            after = jnp.dot(high, later, preferred_element_type=F32) + jnp.dot(low, later, preferred_element_type=F32)
            weight = jnp.exp(z - soft - after - suffix)
            if masked:
                weight = jnp.where(causal, weight, 0.0)
            acc = acc + jnp.dot(weight.astype(BF16), kv[slot, 1, :, kv_at], preferred_element_type=F32)
            return acc, suffix + after[:, 0:1] + soft[:, 0:1]

        acc, suffix = visit(sp, True, jnp.zeros((toks, HEAD_DIM), F32), jnp.zeros((toks, 1), F32))
        acc, suffix = lax.fori_loop(
            0, sp, lambda i, c, visit=visit: visit(sp - 1 - i, False, c[0], c[1]), (acc, suffix)
        )
        ext[pl.ds(HALO, toks), cols] = acc
        logw_ref[:, h : h + 1] = jnp.log(jnp.maximum(1.0 - jnp.exp(-suffix), 0.05))
    for i, g in enumerate(order):
        attn[pl.ds(i * rows, rows)] = ext[pl.ds(pl.multiple_of(HALO + g * rows, HALO), rows), 0 : attn.shape[1]].astype(BF16)

    def block_of(i):
        return ring(pos - (i + 1) // 2) if i % 2 else ring(pos + i // 2)

    def d2d_copy(i):
        return push(snd.at[i], d2d.at[i], d2d_sem.at[0, i], d2d_sem.at[1, i], {"tp": near})

    def x_copy(i):
        return push(xsnd.at[i], xrcv.at[i], x_sem.at[0, i], x_sem.at[1, i], {"tp": far})

    def first(i):
        j = block_of(i)
        wa, wc_ = (woa_ref[...], woc_ref[...]) if i == 0 else (wo[j, 0], wo[j, 1])
        share = lax.dot_general(attn[...], wa, NT, preferred_element_type=F32)
        share = (share + lax.dot_general(conv[...], wc_, NT, preferred_element_type=F32)).astype(BF16)
        snd[i] = share[2 * rows :]
        keep[i] = share[: 2 * rows]
        d2d_copy(i).start()

    def second(i):
        d2d_copy(i).wait_recv()
        xsnd[i] = (keep[i, pl.ds(rows, rows)].astype(F32) + d2d[i, pl.ds(rows, rows)].astype(F32)).astype(BF16)
        x_copy(i).start()

    def third(i):
        x_copy(i).wait_recv()
        own = keep[i, pl.ds(0, rows)].astype(F32) + d2d[i, pl.ds(0, rows)].astype(F32)
        out_ref[block_of(i)] = (own + xrcv[i].astype(F32)).astype(BF16)

    served = 2
    for i in range(n):
        need = (i + 1) // 2
        if need > served:
            serve(wo, w_sem, own_w, need)
            served = need
        first(i)
        if i >= 1:
            second(i - 1)
        if i >= 3:
            third(i - 3)
    second(n - 1)
    for i in range(max(n - 3, 0), n):
        third(i)

    for copy in (*to_far, to_near, *relay, halo):
        copy.wait_send()
    for buf, sem, own in ((wo, w_sem, own_w), (kv, kv_sem, None)):
        for k in range(n - 1):
            for way in range(2):
                hop(buf, sem, way, k, own).wait_send()
    for i in range(n):
        d2d_copy(i).wait_send()
        x_copy(i).wait_send()


def local(
    n, tokens, norm_gain, w_query, w_key, w_value, score_shift, w_conv_b, w_conv_c, w_conv_u,
    conv_kernel, w_out_att, w_out_conv,
):
    rows, d = tokens.shape
    toks = 4 * rows
    feats, att_cols = w_out_att.shape
    conv_cols = w_out_conv.shape[1]
    heads = score_shift.shape[0]
    kv_cols = w_key.shape[1]
    vmem = pl.BlockSpec(memory_space=pltpu.VMEM)
    smem = pl.BlockSpec(memory_space=pltpu.SMEM)
    hbm = pl.BlockSpec(memory_space=pl.ANY)
    dma = pltpu.SemaphoreType.DMA
    out, logw = pl.pallas_call(
        functools.partial(kernel, n),
        out_shape=(
            jax.ShapeDtypeStruct((n, rows, feats), BF16),
            jax.ShapeDtypeStruct((toks, heads), F32),
        ),
        in_specs=[vmem, vmem, hbm, hbm, hbm, smem, hbm, hbm, hbm, vmem, vmem, vmem],
        out_specs=(vmem, vmem),
        scratch_shapes=[
            *[pltpu.VMEM(w.shape, BF16) for w in (w_query, w_key, w_value, w_conv_b, w_conv_c, w_conv_u)],
            pltpu.VMEM((4, rows, d), BF16),
            pltpu.VMEM((2 * rows, d), BF16),
            pltpu.VMEM((toks, w_query.shape[1]), BF16),
            pltpu.VMEM((n, 2, toks, kv_cols), BF16),
            pltpu.VMEM((n, 2, feats, att_cols), BF16),
            pltpu.VMEM((toks, conv_cols), BF16),
            pltpu.VMEM((toks, conv_cols), BF16),
            pltpu.VMEM((HALO, conv_cols), BF16),
            pltpu.VMEM((toks + HALO, max(conv_cols, att_cols)), F32),
            pltpu.VMEM((toks, att_cols), BF16),
            pltpu.VMEM((toks, conv_cols), BF16),
            pltpu.VMEM((n, 2 * rows, feats), BF16),
            pltpu.VMEM((n, 2 * rows, feats), BF16),
            pltpu.VMEM((n, 2 * rows, feats), BF16),
            pltpu.VMEM((n, rows, feats), BF16),
            pltpu.VMEM((n, rows, feats), BF16),
            dma((6,)), dma((5,)), dma((5,)), dma((2, 2, n - 1)), dma((2, 2, n - 1)), dma((2,)), dma((2, n)), dma((2, n)),
        ],
        compiler_params=pltpu.CompilerParams(
            collective_id=0, has_side_effects=True, vmem_limit_bytes=60 * 1024 * 1024
        ),
    )(
        tokens, norm_gain.reshape(1, d), w_query, w_key, w_value, score_shift.reshape(1, heads),
        w_conv_b, w_conv_c, w_conv_u, conv_kernel, w_out_att, w_out_conv,
    )
    return (out.transpose(1, 0, 2).reshape(rows, n * feats), logw)


def solution(mesh):
    return jax.shard_map(
        functools.partial(local, mesh.shape["sp"]),
        mesh=mesh,
        in_specs=(
            P(("sp", "tp"), None), P(), P(None, "tp"), P(None, "tp"), P(None, "tp"), P("tp"),
            P(None, "tp"), P(None, "tp"), P(None, "tp"), P(None, "tp"), P("sp", "tp"), P("sp", "tp"),
        ),
        out_specs=(P(("sp", "tp"), None), P("sp", "tp")),
        check_vma=False,
    )
```

```python
import functools

import jax
import jax.numpy as jnp
from jax import lax
from jax.experimental import pallas as pl
from jax.experimental.pallas import tpu as pltpu
from jax.sharding import PartitionSpec as P

HEAD_DIM = 128
CONV_K = 3
HALO = 16
F32 = jnp.float32
BF16 = jnp.bfloat16
MESH = pl.DeviceIdType.MESH
NT = (((1,), (1,)), ((), ()))


def softplus(z):
    u = jnp.exp(-jnp.abs(z))
    small = u * (1.0 - u * (0.5 - u * (1.0 / 3.0 - u * 0.25)))
    return jnp.maximum(z, 0.0) + jnp.where(u < 0.01, small, jnp.log(1.0 + u))


def kernel(
    n,
    tok_ref, gain_ref, wq_hbm, wk_hbm, wv_hbm, shift_ref, wb_hbm, wc_hbm, wu_hbm, taps_ref, woa_ref, woc_ref,
    out_ref, logw_ref,
    wq, wk, wv, wb, wc, wu, xall, normed, q_sc, kv, wo, gate_sc, prod_sc, prev, ext, attn, conv, partial, totals,
    snd, keep, d2d, xsnd, xrcv,
    load_sem, tok_ssem, tok_rsem, kv_sem, w_sem, halo_sem, d2d_sem, x_sem,
):
    sp = lax.axis_index("sp")
    t = lax.axis_index("tp")
    near = t + 1 - 2 * (t % 2)
    far = t + 2 - 4 * ((t // 2) % 2)
    diag = near + 2 - 4 * ((near // 2) % 2)
    pos = jnp.where(sp % 2 == 0, sp // 2, n - 1 - sp // 2)

    def ring(place):
        place = (place + 2 * n) % n
        return jnp.where(place < n // 2, 2 * place, 2 * (n - 1 - place) + 1)

    right, left = ring(pos + 1), ring(pos - 1)
    following, leading = (sp + 1) % n, (sp + n - 1) % n
    rows = tok_ref.shape[0]
    toks = 4 * rows
    half = rows // 2
    fpart = wo.shape[2] // 2
    heads = q_sc.shape[1] // HEAD_DIM
    kv_cols = kv.shape[4]
    grouping = heads // (kv_cols // HEAD_DIM)

    loads = [
        pltpu.make_async_copy(src, dst, load_sem.at[i])
        for i, (src, dst) in enumerate(
            ((wk_hbm, wk), (wv_hbm, wv), (wq_hbm, wq), (wc_hbm, wc), (wu_hbm, wu), (wb_hbm, wb))
        )
    ]
    own_loads = [
        pltpu.make_async_copy(src, wo.at[sp, i], load_sem.at[6 + i]) for i, src in enumerate((woa_ref, woc_ref))
    ]
    barrier = pltpu.get_barrier_semaphore()
    for place in (right, left, following, leading):
        pl.semaphore_signal(barrier, inc=1, device_id={"sp": place}, device_id_type=MESH)
    for place in (near, far):
        pl.semaphore_signal(barrier, inc=1, device_id={"tp": place}, device_id_type=MESH)
    for load in (*own_loads, *loads):
        load.start()
    pl.semaphore_wait(barrier, 6)

    def push(src, dst, ssem, rsem, who):
        return pltpu.make_async_remote_copy(
            src_ref=src, dst_ref=dst, send_sem=ssem, recv_sem=rsem, device_id=who, device_id_type=MESH
        )

    to_far = [
        push(tok_ref.at[pl.ds(c * half, half)], xall.at[t, pl.ds(c * half, half)], tok_ssem.at[c], tok_rsem.at[c], {"tp": far})
        for c in range(2)
    ]
    to_near = push(tok_ref, xall.at[t], tok_ssem.at[2], tok_rsem.at[2], {"tp": near})
    relay = [
        push(xall.at[far, pl.ds(c * half, half)], xall.at[far, pl.ds(c * half, half)], tok_ssem.at[3 + c], tok_rsem.at[3 + c], {"tp": near})
        for c in range(2)
    ]
    for copy in to_far:
        copy.start()
    to_near.start()

    last = n // 2

    def hop(part, sem, way, step, chunk):
        block = ring(pos - (step - 1)) if way == 0 else ring(pos + (step - 1))
        view = part(block, chunk, step)
        return push(
            view[0], view[1], sem.at[0, way, step - 1, chunk], sem.at[1, way, step - 1, chunk],
            {"sp": right if way == 0 else left},
        )

    def ways(step, chunk, chunks):
        if isinstance(step, int) and step == last:
            return (0,) if chunk < chunks // 2 else (1,)
        return (0, 1)

    early = t // 2

    def kv_part(block, chunk, step):
        view = kv.at[block, early + chunk * (1 - 2 * early)]
        return view, view

    def w_part(block, chunk, step):
        view = wo.at[block, chunk // 2, pl.ds(pl.multiple_of((chunk % 2) * fpart, fpart), fpart)]
        return view, view

    rings = {"kv": (kv_part, kv_sem, 2), "w": (w_part, w_sem, 4)}

    def emit(name, step, chunk):
        part, sem, chunks = rings[name]
        for way in ways(step, chunk, chunks):
            hop(part, sem, way, step, chunk).start()

    def take(name, step, chunk, onward=None):
        part, sem, chunks = rings[name]
        for way in ways(step, chunk, chunks):
            hop(part, sem, way, step, chunk).wait_recv()
        if onward or (onward is None and step < last):
            emit(name, step + 1, chunk)

    for load in own_loads:
        load.wait()
    for chunk in (0, 1):
        emit("w", 1, chunk)

    def dot(w):
        return jnp.dot(normed[...], w[...], preferred_element_type=F32).astype(BF16)

    def project_kv(groups, pair):
        for i, g in enumerate(groups):
            x = (tok_ref[...] if g is None else xall[g]).astype(F32)
            inverse = lax.rsqrt(jnp.mean(x * x, axis=-1, keepdims=True) + 1e-06)
            at = rows * (t % 2 if i == 0 else 1 - t % 2)
            normed[pl.ds(pl.multiple_of(at, rows), rows)] = (x * inverse * gain_ref[...]).astype(BF16)
        kv[sp, pair, 0] = dot(wk)
        kv[sp, pair, 1] = dot(wv)

    def project_rest(pair):
        at = pl.ds(pl.multiple_of(pair * 2 * rows, 2 * rows), 2 * rows)
        prod_sc[at] = (dot(wc).astype(F32) * dot(wu).astype(F32)).astype(BF16)
        q_sc[at] = dot(wq)
        gate_sc[at] = dot(wb)

    to_near.wait_recv()
    for load in loads[:2]:
        load.wait()
    project_kv((None, near), early)
    emit("kv", 1, 0)
    for chunk in (2, 3):
        emit("w", 1, chunk)
    for load in loads[2:]:
        load.wait()
    project_rest(early)
    to_far[0].wait_recv()
    relay[0].start()
    take("kv", 1, 0)
    take("w", 1, 0)
    to_far[1].wait_recv()
    relay[1].start()
    for c in range(2):
        relay[c].wait_recv()
    project_kv((far, diag), 1 - early)
    emit("kv", 1, 1)
    take("w", 1, 1)
    project_rest(1 - early)
    halo = push(prod_sc.at[pl.ds(toks - HALO, HALO)], prev, halo_sem.at[0], halo_sem.at[1], {"sp": following})
    halo.start()

    key_i = lax.broadcasted_iota(jnp.int32, (toks, toks), 0)
    key_j = lax.broadcasted_iota(jnp.int32, (toks, toks), 1)
    later = (key_i > key_j).astype(F32).astype(BF16)
    lane = lax.broadcasted_iota(jnp.int32, (toks, totals.shape[2]), 1)
    scale = HEAD_DIM ** (-0.5)
    order = (t, far, near, diag)

    def visit(slot, masked):
        for h in range(heads):
            cols = pl.ds(h * HEAD_DIM, HEAD_DIM)
            kv_at = pl.ds((h // grouping) * HEAD_DIM, HEAD_DIM)
            keys = kv[slot, :, 0, :, kv_at].reshape(toks, HEAD_DIM)
            vals = kv[slot, :, 1, :, kv_at].reshape(toks, HEAD_DIM)
            z = lax.dot_general(q_sc[:, cols], keys, NT, preferred_element_type=F32) * scale + shift_ref[0, h]
            soft = softplus(z)
            if masked:
                soft = jnp.where(key_j < key_i, soft, 0.0)
            high = soft.astype(BF16)
            low = (soft - high.astype(F32)).astype(BF16)
            after = jnp.dot(high, later, preferred_element_type=F32) + jnp.dot(low, later, preferred_element_type=F32)
            weight = jnp.exp(z - soft - after)
            if masked:
                weight = jnp.where(key_j < key_i, weight, 0.0)
            partial[slot, :, cols] = jnp.dot(weight.astype(BF16), vals, preferred_element_type=F32)
            total = after[:, 0:1] + soft[:, 0:1]
            totals[h] = jnp.where(lane == slot, total, totals[h])

    def visit_at(step, both=True):
        def side(i, carry):
            slot = ring(pos + (2 * i - 1) * step)

            @pl.when(slot < sp)
            def _():
                visit(slot, False)

            return carry

        lax.fori_loop(0, 2 if both else 1, side, 0)

    totals[...] = jnp.zeros(totals.shape, F32)
    visit(sp, True)

    def w_event(m):
        return m // 4 + 1, m % 4

    def body(s, carry):
        if n > 4:
            take("kv", s + 1, 0, True)
            take("kv", s, 1, True)
            visit_at(s)
            take("w", *w_event(2 * s), True)
            take("w", *w_event(2 * s + 1), True)
        return carry

    def convolve():
        halo.wait_recv()
        ext[pl.ds(HALO, toks)] = prod_sc[...].astype(F32)
        ext[pl.ds(0, HALO)] = jnp.where(sp == 0, 0.0, prev[...].astype(F32))
        summed = jnp.zeros((toks, ext.shape[1]), F32)
        for tap in range(CONV_K):
            summed = summed + taps_ref[tap : tap + 1, :] * ext[pl.ds(HALO - (CONV_K - 1) + tap, toks)]
        ext[pl.ds(HALO, toks)] = gate_sc[...].astype(F32) * summed
        for i, g in enumerate(order):
            conv[pl.ds(i * rows, rows)] = ext[pl.ds(pl.multiple_of(HALO + g * rows, HALO), rows)].astype(BF16)

    loops = max(last - 3, 0)
    lax.fori_loop(1, 1 + loops, body, 0)
    w_done = 2 + 2 * loops
    convolve()
    for s in range(1 + loops, last + 1):
        if s + 1 <= last:
            take("kv", s + 1, 0)
        take("kv", s, 1)
        visit_at(s, s < last)
        if s < last:
            for m in (w_done, w_done + 1):
                take("w", *w_event(m))
            w_done += 2

    def combine(i, carry):
        slot = sp - i
        suffixes = []
        for h in range(heads):
            cols = pl.ds(h * HEAD_DIM, HEAD_DIM)
            suffix = carry[h]
            ext[pl.ds(HALO, toks), cols] += jnp.exp(-suffix) * partial[slot, :, cols]
            total = jnp.sum(jnp.where(lane == slot, totals[h], 0.0), axis=1, keepdims=True)
            suffixes.append(suffix + total)
        return tuple(suffixes)

    ext[...] = jnp.zeros(ext.shape, F32)
    suffixes = lax.fori_loop(0, sp + 1, combine, tuple(jnp.zeros((toks, 1), F32) for _ in range(heads)))
    for h in range(heads):
        spread = jnp.broadcast_to(suffixes[h], (toks, 128)).T[0:1, :]
        logw_ref[h : h + 1, :] = jnp.log(jnp.maximum(1.0 - jnp.exp(-spread), 0.05))
    for i, g in enumerate(order):
        attn[pl.ds(i * rows, rows)] = ext[pl.ds(pl.multiple_of(HALO + g * rows, HALO), rows), 0 : attn.shape[1]].astype(BF16)

    def block_of(i):
        return ring(pos - (i + 1) // 2) if i % 2 else ring(pos + i // 2)

    def d2d_copy(i):
        return push(snd.at[i], d2d.at[i], d2d_sem.at[0, i], d2d_sem.at[1, i], {"tp": near})

    def x_copy(i):
        return push(xsnd.at[i], xrcv.at[i], x_sem.at[0, i], x_sem.at[1, i], {"tp": far})

    def first(i):
        j = block_of(i)
        share = lax.dot_general(attn[...], wo[j, 0], NT, preferred_element_type=F32)
        share = (share + lax.dot_general(conv[...], wo[j, 1], NT, preferred_element_type=F32)).astype(BF16)
        snd[i] = share[2 * rows :]
        keep[i] = share[: 2 * rows]
        d2d_copy(i).start()

    def second(i):
        d2d_copy(i).wait_recv()
        xsnd[i] = (keep[i, pl.ds(rows, rows)].astype(F32) + d2d[i, pl.ds(rows, rows)].astype(F32)).astype(BF16)
        x_copy(i).start()

    def third(i):
        x_copy(i).wait_recv()
        own = keep[i, pl.ds(0, rows)].astype(F32) + d2d[i, pl.ds(0, rows)].astype(F32)
        done = (own + xrcv[i].astype(F32)).astype(BF16)
        if len(out_ref.shape) == 3:
            out_ref[block_of(i)] = done
        else:
            feats = keep.shape[2]
            out_ref[:, pl.ds(pl.multiple_of(block_of(i) * feats, feats), feats)] = done

    for i in range(n):
        while w_done < 4 * ((i + 1) // 2):
            take("w", *w_event(w_done))
            w_done += 1
        first(i)
        if i >= 1:
            second(i - 1)
        if i >= 3:
            third(i - 3)
    second(n - 1)
    for i in range(max(n - 3, 0), n):
        third(i)

    for copy in (*to_far, to_near, *relay, halo):
        copy.wait_send()
    for part, sem, chunks in rings.values():
        for step in range(1, last + 1):
            for chunk in range(chunks):
                for way in ways(step, chunk, chunks):
                    hop(part, sem, way, step, chunk).wait_send()
    for i in range(n):
        d2d_copy(i).wait_send()
        x_copy(i).wait_send()


def local(
    n, tokens, norm_gain, w_query, w_key, w_value, score_shift, w_conv_b, w_conv_c, w_conv_u,
    conv_kernel, w_out_att, w_out_conv,
):
    rows, d = tokens.shape
    toks = 4 * rows
    feats, att_cols = w_out_att.shape
    conv_cols = w_out_conv.shape[1]
    heads = score_shift.shape[0]
    kv_cols = w_key.shape[1]
    vmem = pl.BlockSpec(memory_space=pltpu.VMEM)
    smem = pl.BlockSpec(memory_space=pltpu.SMEM)
    hbm = pl.BlockSpec(memory_space=pl.ANY)
    dma = pltpu.SemaphoreType.DMA
    wide = feats % 128 == 0
    out, logw = pl.pallas_call(
        functools.partial(kernel, n),
        out_shape=(
            jax.ShapeDtypeStruct((rows, n * feats) if wide else (n, rows, feats), BF16),
            jax.ShapeDtypeStruct((heads, toks), F32),
        ),
        in_specs=[vmem, vmem, hbm, hbm, hbm, smem, hbm, hbm, hbm, vmem, hbm, hbm],
        out_specs=(vmem, vmem),
        scratch_shapes=[
            *[pltpu.VMEM(w.shape, BF16) for w in (w_query, w_key, w_value, w_conv_b, w_conv_c, w_conv_u)],
            pltpu.VMEM((4, rows, d), BF16),
            pltpu.VMEM((2 * rows, d), BF16),
            pltpu.VMEM((toks, w_query.shape[1]), BF16),
            pltpu.VMEM((n, 2, 2, 2 * rows, kv_cols), BF16),
            pltpu.VMEM((n, 2, feats, att_cols), BF16),
            pltpu.VMEM((toks, conv_cols), BF16),
            pltpu.VMEM((toks, conv_cols), BF16),
            pltpu.VMEM((HALO, conv_cols), BF16),
            pltpu.VMEM((toks + HALO, max(conv_cols, att_cols)), F32),
            pltpu.VMEM((toks, att_cols), BF16),
            pltpu.VMEM((toks, conv_cols), BF16),
            pltpu.VMEM((n, toks, att_cols), F32),
            pltpu.VMEM((heads, toks, 128), F32),
            pltpu.VMEM((n, 2 * rows, feats), BF16),
            pltpu.VMEM((n, 2 * rows, feats), BF16),
            pltpu.VMEM((n, 2 * rows, feats), BF16),
            pltpu.VMEM((n, rows, feats), BF16),
            pltpu.VMEM((n, rows, feats), BF16),
            dma((8,)), dma((5,)), dma((5,)), dma((2, 2, n // 2, 2)), dma((2, 2, n // 2, 4)), dma((2,)), dma((2, n)), dma((2, n)),
        ],
        compiler_params=pltpu.CompilerParams(
            collective_id=0, has_side_effects=True, vmem_limit_bytes=60 * 1024 * 1024
        ),
    )(
        tokens, norm_gain.reshape(1, d), w_query, w_key, w_value, score_shift.reshape(1, heads),
        w_conv_b, w_conv_c, w_conv_u, conv_kernel, w_out_att, w_out_conv,
    )
    if not wide:
        out = out.transpose(1, 0, 2).reshape(rows, n * feats)
    return (out, logw.T)


def solution(mesh):
    return jax.shard_map(
        functools.partial(local, mesh.shape["sp"]),
        mesh=mesh,
        in_specs=(
            P(("sp", "tp"), None), P(), P(None, "tp"), P(None, "tp"), P(None, "tp"), P("tp"),
            P(None, "tp"), P(None, "tp"), P(None, "tp"), P(None, "tp"), P("sp", "tp"), P("sp", "tp"),
        ),
        out_specs=(P(("sp", "tp"), None), P("sp", "tp")),
        check_vma=False,
    )
```
